32 devices in a mesh: fs: 8 (over z, y), tp: 4 (over x, core).
Axes of the slice: x: 2, y: 2, z: 4, core: 2. Of those that a mesh axis runs over, the one named last changes fastest.
Arguments:
- tokens: bfloat16 [12288, 2048], P('fs', 'tp'), may hold values from -6 to 6
- norm_gain: float32 [2048], P('fs'), may hold values from 0.1 to 1.9
- up_weight: float32 [2048, 8192], P('fs', 'tp'), may hold values from -0.125 to 0.125
- down_weight: float32 [2048, 8192], P('fs', 'tp'), may hold values from -0.0625 to 0.0625
Outputs:
- up_matrix: bfloat16 [2048, 8192], P(None, 'tp')
- down_matrix: bfloat16 [2048, 8192], P(None, 'tp')
- mixed: bfloat16 [12288, 2048], P('fs', 'tp')
The draws below stay inside these ranges and needn't reach their ends.
All inputs are finite; a program needn't handle non-finite values.
Results may differ from the reference program's by a relative error of at most 0.0095.
Values may be sent and summed in bfloat16 or wider, within the bound.
A program may use at most 128 MiB of HBM per device.

```python
import jax
import jax.numpy as jnp
from jax import lax

D = 2048
FF = 8192
TOKENS = 12288
N_TP = 4


def levels(rng, shape, pieces, smallest, high):
    factor_of, own = 1.0, jax.random.fold_in(rng, 6)
    for dim, parts in pieces:
        draws = jnp.exp(jax.random.uniform(jax.random.fold_in(own, dim), (parts,), jnp.float32, smallest / len(pieces), high / len(pieces)))
        factor_of = factor_of * jnp.repeat(draws, shape[dim] // parts).reshape([-1 if axis == dim else 1 for axis in range(len(shape))])
    return factor_of


def bell_draw(stream_key, dims, deviation, most, pieces=(), kind=jnp.bfloat16):
    loudness = levels(stream_key, dims, pieces, -0.22, 0.18) if pieces else 1.0
    drawn = jax.random.normal(stream_key, dims, jnp.float32) * deviation * loudness
    return jnp.minimum(jnp.maximum(drawn, -most), most).astype(kind)


def setup_inputs(seed: int = 0) -> dict:
    arg_keys = jax.random.split(jax.random.key(seed), 5)
    tokens = bell_draw(arg_keys[0], (TOKENS, D), 1.0, 6.0, ((0, 8), (1, 4)))
    norm_gain = jnp.clip(1.0 + 0.18 * jax.random.normal(arg_keys[1], (D,), jnp.float32), 0.1, 1.9)
    up_weight = bell_draw(arg_keys[2], (D, FF), D ** -0.5, 0.125, ((0, 8), (1, 4)), jnp.float32)
    down_weight = bell_draw(arg_keys[3], (D, FF), FF ** -0.5, 0.0625, ((0, 8), (1, 4)), jnp.float32)
    return dict(tokens=tokens, norm_gain=norm_gain, up_weight=up_weight, down_weight=down_weight)


epsilon = 1e-06

def reference(tokens, norm_gain, up_weight, down_weight):
    up_matrix = (norm_gain[:, None] * up_weight).astype(jnp.bfloat16)
    down_matrix = down_weight.astype(jnp.bfloat16)
    widened = tokens.astype(jnp.float32)
    normed = (widened * lax.rsqrt(lax.optimization_barrier(jnp.mean(widened * widened, axis=-1, keepdims=True)) + epsilon)).astype(jnp.bfloat16)
    width = FF // N_TP
    mixed_sum = jnp.zeros((tokens.shape[0], tokens.shape[1]), jnp.float32)
    for group_index in range(N_TP):
        up_block = up_matrix[:, group_index * width:(group_index + 1) * width]
        down_block = down_matrix[:, group_index * width:(group_index + 1) * width]
        up_values = jnp.dot(normed, up_block, preferred_element_type=jnp.float32)
        hidden = jnp.square(jax.nn.relu(up_values)).astype(jnp.bfloat16)
        partial_value = lax.dot_general(hidden, down_block, (((1,), (1,)), ((), ())), preferred_element_type=jnp.float32)
        mixed_sum = mixed_sum + partial_value.astype(jnp.bfloat16).astype(jnp.float32)
    return (up_matrix, down_matrix, mixed_sum.astype(jnp.bfloat16))
```

```python
import functools

import jax
import jax.numpy as jnp
from jax import lax
from jax.experimental import pallas as pl
from jax.experimental.pallas import tpu as pltpu
from jax.sharding import PartitionSpec as P

epsilon = 1e-06
MESH = pl.DeviceIdType.MESH
UP, DOWN, SIDE = 0, 1, 2


def chunks_of(rows):
    extra = max(16, rows // 8 // 16 * 16)
    main = rows - extra
    if main % 32 == 0:
        half = main // 2
        return [(0, half), (half, half), (main, extra)]
    return [(0, main), (main, extra)]


def kernel(n, tp, tok_in, upl, downl, up_out, down_out, mixed_out,
           tok, up, down, hidden, part, pair, cross, total,
           send_sem, recv_sem, tok_send, tok_recv, pair_send, pair_recv, cross_send, cross_recv, local_sem):
    rows = upl.shape[0]
    tokens, width = tok_in.shape
    chain = n // 2
    groups = tp // 2
    per_owner = n // tp
    chunks = chunks_of(rows)
    extra = len(chunks) - 1
    mains = range(extra)
    fs, me = lax.axis_index("fs"), lax.axis_index("tp")
    z, y = fs // 2, fs % 2
    group, core = me // 2, me % 2
    partner = group * 2 + 1 - core
    bufs = (up, down)
    mine = (upl, downl)

    def target(way):
        if way == UP:
            return {"fs": jnp.minimum(z + 1, chain - 1) * 2 + y}
        if way == DOWN:
            return {"fs": jnp.maximum(z - 1, 0) * 2 + y}
        return {"fs": z * 2 + 1 - y}

    def spot(src, k):
        return pl.ds(pl.multiple_of(src * rows, 16) + chunks[k][0], chunks[k][1])

    def copy(m, src, k, way, own):
        where = spot(src, k)
        return pltpu.make_async_remote_copy(
            src_ref=mine[m].at[pl.ds(*chunks[k])] if own else bufs[m].at[where],
            dst_ref=bufs[m].at[where],
            send_sem=send_sem.at[m, way, src, k],
            recv_sem=recv_sem.at[m, src, k],
            device_id=target(way),
            device_id_type=MESH,
        )

    def arrived(m, src, k):
        where = spot(src, k)
        pltpu.make_async_remote_copy(
            src_ref=bufs[m].at[where], dst_ref=bufs[m].at[where],
            send_sem=send_sem.at[m, SIDE, src, k], recv_sem=recv_sem.at[m, src, k],
            device_id=target(SIDE), device_id_type=MESH,
        ).wait_recv()

    def own_sends(m):
        order = [(SIDE, extra)] + [(way, k) for k in mains for way in (UP, DOWN, SIDE)] + [(UP, extra), (DOWN, extra)]
        return [(way, k) for way, k in order]

    def when_way(way, fn):
        if way == UP:
            pl.when(z < chain - 1)(fn)
        elif way == DOWN:
            pl.when(z > 0)(fn)
        else:
            fn()

    def start_own(m):
        for way, k in own_sends(m):
            when_way(way, lambda way=way, k=k: copy(m, fs, k, way, True).start())

    def relay_own_extra(m, act):
        other = z * 2 + 1 - y
        for way in (UP, DOWN):
            when_way(way, lambda way=way: act(copy(m, other, extra, way, False)))

    def step_sends(m, d, act, wait):
        plan = [(k, 0) for k in mains] + [(extra, 0), (extra, 1)]
        for k, flip in plan:
            for sign, way in ((-1, UP), (1, DOWN)):
                at = z + sign * d
                src = at * 2 + (y + flip) % 2

                @pl.when((at >= 0) & (at < chain))
                def _():
                    if wait:
                        arrived(m, src, k)
                    when_way(way, lambda: act(copy(m, src, k, way, False)))
                    if k != extra:
                        act(copy(m, src, k, SIDE, False))

    def side_arrivals(m, d):
        for sign in (-1, 1) if not (isinstance(d, int) and d == 0) else (1,):
            at = z + sign * d

            @pl.when((at >= 0) & (at < chain))
            def _():
                for k in mains:
                    arrived(m, at * 2 + 1 - y, k)

    barrier = pltpu.get_barrier_semaphore()
    greet = [{"fs": lax.rem(z + 1, chain) * 2 + y}, {"fs": lax.rem(z + chain - 1, chain) * 2 + y},
             {"fs": z * 2 + 1 - y}, {"tp": partner}]
    greet += [{"tp": lax.rem(group + g, groups) * 2 + core} for g in range(1, groups)]
    for who in greet:
        pl.semaphore_signal(barrier, inc=1, device_id=who, device_id_type=MESH)
    pl.semaphore_wait(barrier, len(greet))

    start_own(0)

    def columns(owner):
        return pl.ds(pl.multiple_of(owner * width, 128), width)

    def token_copy(owner, to, slot, own):
        return pltpu.make_async_remote_copy(
            src_ref=tok_in if own else tok.at[:, columns(owner)],
            dst_ref=tok.at[:, columns(owner)],
            send_sem=tok_send.at[slot], recv_sem=tok_recv.at[owner],
            device_id={"tp": to}, device_id_type=MESH)

    across = [lax.rem(group + g, groups) * 2 + core for g in range(1, groups)]
    back = [lax.rem(group + groups - g, groups) * 2 + core for g in range(1, groups)]
    token_sends = [token_copy(me, to, i, True) for i, to in enumerate(across)]
    token_sends.append(token_copy(me, partner, groups - 1, True))
    for c in token_sends:
        c.start()
    own_tokens = pltpu.make_async_copy(tok_in, tok.at[:, columns(me)], local_sem.at[0])
    own_tokens.start()
    own_rows = pl.ds(pl.multiple_of(fs * rows, 16), rows)
    own_up = pltpu.make_async_copy(upl, up.at[own_rows], local_sem.at[1])
    own_up.start()
    own_down = pltpu.make_async_copy(downl, down.at[own_rows], local_sem.at[2])
    own_down.start()

    arrived(0, z * 2 + 1 - y, extra)
    relay_own_extra(0, lambda c: c.start())
    step_sends(0, 1, lambda c: c.start(), True)

    relays = []
    for i, owner in enumerate(back):
        token_copy(owner, partner, groups + i, False).wait_recv()
        c = token_copy(owner, partner, groups + i, False)
        c.start()
        relays.append(c)
    token_copy(partner, partner, 0, False).wait_recv()
    for g in range(1, groups):
        token_copy(lax.rem(group + g, groups) * 2 + 1 - core, partner, 0, False).wait_recv()
    for c in token_sends + relays:
        c.wait_send()
    own_tokens.wait()
    tile = 128

    @pl.loop(0, tokens // tile)
    def _(i):
        at = pl.ds(pl.multiple_of(i * tile, tile), tile)
        wide = tok[at, :].astype(jnp.float32)
        scale = lax.rsqrt(jnp.mean(wide * wide, axis=-1, keepdims=True) + epsilon)
        tok[at, :] = (wide * scale).astype(jnp.bfloat16)

    for d in range(2, chain):
        step_sends(0, d, lambda c: c.start(), True)
    start_own(1)
    for d in range(chain):
        side_arrivals(0, d)
    arrived(1, z * 2 + 1 - y, extra)
    relay_own_extra(1, lambda c: c.start())
    step_sends(1, 1, lambda c: c.start(), True)
    own_up.wait()
    up_write = pltpu.make_async_copy(up, up_out, local_sem.at[1])
    up_write.start()

    bm, bn = min(512, tokens), min(512, up.shape[1])

    @pl.loop(0, up.shape[1] // bn)
    def _(j):
        cols = pl.ds(pl.multiple_of(j * bn, bn), bn)

        @pl.loop(0, tokens // bm)
        def _(i):
            at = pl.ds(pl.multiple_of(i * bm, bm), bm)
            values = jnp.dot(tok[at, :], up[:, cols], preferred_element_type=jnp.float32)
            values = jnp.maximum(values, 0.0)
            hidden[at, cols] = (values * values).astype(jnp.bfloat16)

    def pair_copy(r):
        return pltpu.make_async_remote_copy(
            src_ref=part.at[r], dst_ref=pair.at[r], send_sem=pair_send.at[r], recv_sem=pair_recv.at[r],
            device_id={"tp": partner}, device_id_type=MESH)

    def cross_copy(r, to_group, from_group):
        return pltpu.make_async_remote_copy(
            src_ref=part.at[r], dst_ref=cross.at[from_group, r % per_owner],
            send_sem=cross_send.at[r], recv_sem=cross_recv.at[from_group, r % per_owner],
            device_id={"tp": to_group * 2 + core}, device_id_type=MESH)

    def block_write(r):
        where = pl.ds(pl.multiple_of(r * rows, 16), rows)
        return pltpu.make_async_copy(down.at[where], down_out.at[where], local_sem.at[3 + r])

    def multiply(r):
        block_write(r).start()
        where = pl.ds(pl.multiple_of(r * rows, 16), rows)

        @pl.loop(0, tokens // bm)
        def _(i):
            at = pl.ds(pl.multiple_of(i * bm, bm), bm)
            part[r, at, :] = lax.dot_general(
                hidden[at, :], down[where, :], (((1,), (1,)), ((), ())),
                preferred_element_type=jnp.float32).astype(jnp.bfloat16)

        @pl.when(r // per_owner % 2 != core)
        def _():
            pair_copy(r).start()

    def pair_sum(r):
        owner = r // per_owner

        @pl.when(owner % 2 == core)
        def _():
            pair_copy(r).wait_recv()

            @pl.loop(0, tokens // tile)
            def _(i):
                at = pl.ds(pl.multiple_of(i * tile, tile), tile)
                both = part[r, at, :].astype(jnp.float32) + pair[r, at, :].astype(jnp.float32)
                part[r, at, :] = both.astype(jnp.bfloat16)

            @pl.when(owner // 2 != group)
            def _():
                cross_copy(r, owner // 2, group).start()

    def at_distance(d, flip, fn):
        for sign in (-1, 1):
            at = z + sign * d

            @pl.when((at >= 0) & (at < chain))
            def _():
                fn(at * 2 + (y + flip) % 2)

    own_down.wait()
    multiply(fs)
    for k in mains:
        arrived(1, z * 2 + 1 - y, k)
    multiply(z * 2 + 1 - y)
    pair_sum(fs)
    at_distance(1, 0, multiply)
    pair_sum(z * 2 + 1 - y)

    @pl.loop(2, chain)
    def _(d):
        step_sends(1, d, lambda c: c.start(), True)
        side_arrivals(1, d - 1)
        at_distance(d - 1, 1, multiply)
        at_distance(d - 1, 0, pair_sum)
        at_distance(d, 0, multiply)
        at_distance(d - 1, 1, pair_sum)

    at_distance(chain - 1, 0, pair_sum)
    side_arrivals(1, chain - 1)
    at_distance(chain - 1, 1, multiply)
    at_distance(chain - 1, 1, pair_sum)

    for s in range(per_owner):
        r = me * per_owner + s
        for g in range(1, groups):
            other = lax.rem(group + g, groups)
            cross_copy(r, other, other).wait_recv()

        @pl.loop(0, tokens // tile)
        def _(i):
            at = pl.ds(pl.multiple_of(i * tile, tile), tile)
            value = part[r, at, :].astype(jnp.float32)
            for g in range(1, groups):
                value = value + cross[lax.rem(group + g, groups), s, at, :].astype(jnp.float32)
            total[at, s * rows:(s + 1) * rows] = value.astype(jnp.bfloat16)

    mixed_write = pltpu.make_async_copy(total, mixed_out, local_sem.at[0])
    mixed_write.start()

    for m in (0, 1):
        for way, k in own_sends(m):
            when_way(way, lambda way=way, k=k: copy(m, fs, k, way, True).wait_send())
        relay_own_extra(m, lambda c: c.wait_send())

        @pl.loop(1, chain)
        def _(d):
            step_sends(m, d, lambda c: c.wait_send(), False)

    @pl.loop(0, n)
    def _(r):
        owner = r // per_owner

        @pl.when(owner % 2 != core)
        def _():
            pair_copy(r).wait_send()

        @pl.when((owner % 2 == core) & (owner // 2 != group))
        def _():
            cross_copy(r, owner // 2, group).wait_send()

        block_write(r).wait()

    up_write.wait()
    mixed_write.wait()


def on_device(n, tp, tokens, norm_gain, up_weight, down_weight):
    up_local = (norm_gain[:, None] * up_weight).astype(jnp.bfloat16)
    down_local = down_weight.astype(jnp.bfloat16)
    rows, units = up_local.shape
    count, width = tokens.shape
    bf16 = jnp.bfloat16
    groups, per_owner = tp // 2, n // tp
    chunks = len(chunks_of(rows))
    features = width * tp
    dma = pltpu.SemaphoreType.DMA
    flops = 2 * 2 * count * features * units
    return tuple(pl.pallas_call(
        functools.partial(kernel, n, tp),
        out_shape=(jax.ShapeDtypeStruct((features, units), bf16), jax.ShapeDtypeStruct((features, units), bf16),
                   jax.ShapeDtypeStruct((count, width), bf16)),
        in_specs=[pl.BlockSpec(memory_space=pltpu.VMEM)] * 3,
        out_specs=[pl.BlockSpec(memory_space=pl.ANY)] * 3,
        scratch_shapes=[
            pltpu.VMEM((count, features), bf16),
            pltpu.VMEM((features, units), bf16),
            pltpu.VMEM((features, units), bf16),
            pltpu.VMEM((count, units), bf16),
            pltpu.VMEM((n, count, rows), bf16),
            pltpu.VMEM((n, count, rows), bf16),
            pltpu.VMEM((groups, per_owner, count, rows), bf16),
            pltpu.VMEM((count, width), bf16),
            dma((2, 3, n, chunks)), dma((2, n, chunks)),
            dma((2 * groups,)), dma((tp,)),
            dma((n,)), dma((n,)), dma((n,)), dma((groups, per_owner)),
            dma((3 + n,)),
        ],
        cost_estimate=pl.CostEstimate(flops=flops, bytes_accessed=4 * features * units * 2, transcendentals=0),
        compiler_params=pltpu.CompilerParams(
            collective_id=0, has_side_effects=True, vmem_limit_bytes=67043328),
    )(tokens, up_local, down_local))


def solution(mesh):
    return jax.shard_map(
        functools.partial(on_device, mesh.shape["fs"], mesh.shape["tp"]),
        mesh=mesh,
        in_specs=(P("fs", "tp"), P("fs"), P("fs", "tp"), P("fs", "tp")),
        out_specs=(P(None, "tp"), P(None, "tp"), P("fs", "tp")),
        check_vma=False,
    )
```

```python
import functools

import jax
import jax.numpy as jnp
from jax import lax
from jax.experimental import pallas as pl
from jax.experimental.pallas import tpu as pltpu
from jax.sharding import PartitionSpec as P

epsilon = 1e-06
MESH = pl.DeviceIdType.MESH
UP, DOWN, SIDE = 0, 1, 2


def chunks_of(rows, m):
    extra = max(16, rows * (2 + m) // 16 // 16 * 16)
    main, half = rows - extra, rows // 2
    if half % 128 == 0:
        return [(0, half), (half, main - half), (main, extra)]
    return [(0, main), (main, extra)]


def kernel(n, tp, tok_in, gain, up_weight, down_weight, up, down, total,
           stage, tok, hidden, part, pair, cross,
           send_sem, recv_sem, tok_send, tok_recv, pair_send, pair_recv, cross_send, cross_recv, local_sem):
    rows, units = up_weight.shape
    tokens, width = tok_in.shape
    chain = n // 2
    groups = tp // 2
    per_owner = n // tp
    chunks = [chunks_of(rows, 0), chunks_of(rows, 1)]
    extra = len(chunks[0]) - 1
    mains = range(extra)
    halves = extra
    half_rows = rows // halves
    fs, me = lax.axis_index("fs"), lax.axis_index("tp")
    z, y = fs // 2, fs % 2
    group, core = me // 2, me % 2
    partner = group * 2 + 1 - core
    bufs = (up, down)

    def target(way):
        if way == UP:
            return {"fs": jnp.minimum(z + 1, chain - 1) * 2 + y}
        if way == DOWN:
            return {"fs": jnp.maximum(z - 1, 0) * 2 + y}
        return {"fs": z * 2 + 1 - y}

    def spot(m, src, k):
        return pl.ds(pl.multiple_of(pl.multiple_of(src * rows, 16) + chunks[m][k][0], 16), chunks[m][k][1])

    def copy(m, src, k, way):
        where = spot(m, src, k)
        return pltpu.make_async_remote_copy(
            src_ref=bufs[m].at[where],
            dst_ref=bufs[m].at[where],
            send_sem=send_sem.at[m, way, src, k],
            recv_sem=recv_sem.at[m, src, k],
            device_id=target(way),
            device_id_type=MESH,
        )

    def arrived(m, src, k):
        where = spot(m, src, k)
        pltpu.make_async_remote_copy(
            src_ref=bufs[m].at[where], dst_ref=bufs[m].at[where],
            send_sem=send_sem.at[m, SIDE, src, k], recv_sem=recv_sem.at[m, src, k],
            device_id=target(SIDE), device_id_type=MESH,
        ).wait_recv()

    def own_sends(m):
        order = [(SIDE, extra)] + [(way, k) for k in mains for way in (UP, DOWN, SIDE)] + [(UP, extra), (DOWN, extra)]
        return [(way, k) for way, k in order]

    def when_way(way, fn):
        if way == UP:
            pl.when(z < chain - 1)(fn)
        elif way == DOWN:
            pl.when(z > 0)(fn)
        else:
            fn()

    def start_own(m):
        for way, k in own_sends(m):
            when_way(way, lambda way=way, k=k: copy(m, fs, k, way).start())

    def relay_own_extra(m, act):
        other = z * 2 + 1 - y
        for way in (UP, DOWN):
            when_way(way, lambda way=way: act(copy(m, other, extra, way)))

    def step_sends(m, d, act, wait):
        plan = [(k, 0) for k in mains] + [(extra, 0), (extra, 1)]
        for k, flip in plan:
            for sign, way in ((-1, UP), (1, DOWN)):
                at = z + sign * d
                src = at * 2 + (y + flip) % 2

                @pl.when((at >= 0) & (at < chain))
                def _():
                    if wait:
                        arrived(m, src, k)
                    when_way(way, lambda: act(copy(m, src, k, way)))
                    if k != extra:
                        act(copy(m, src, k, SIDE))

    def side_arrivals(m, d):
        for sign in (-1, 1) if not (isinstance(d, int) and d == 0) else (1,):
            at = z + sign * d

            @pl.when((at >= 0) & (at < chain))
            def _():
                for k in mains:
                    arrived(m, at * 2 + 1 - y, k)

    own_rows = pl.ds(pl.multiple_of(fs * rows, 16), rows)
    loads = [pltpu.make_async_copy(up_weight, stage.at[0], local_sem.at[1]),
             pltpu.make_async_copy(tok_in, tok.at[:, pl.ds(pl.multiple_of(me * width, 128), width)], local_sem.at[0]),
             pltpu.make_async_copy(down_weight, stage.at[1], local_sem.at[2])]
    for load in loads:
        load.start()

    barrier = pltpu.get_barrier_semaphore()
    greet = [{"fs": lax.rem(z + 1, chain) * 2 + y}, {"fs": lax.rem(z + chain - 1, chain) * 2 + y},
             {"fs": z * 2 + 1 - y}, {"tp": partner}]
    greet += [{"tp": lax.rem(group + g, groups) * 2 + core} for g in range(1, groups)]
    for who in greet:
        pl.semaphore_signal(barrier, inc=1, device_id=who, device_id_type=MESH)
    loads[0].wait()
    by_row = jnp.transpose(jnp.broadcast_to(gain[...], (128, rows)))[:, :1]
    up[own_rows, :] = (by_row * stage[0]).astype(jnp.bfloat16)
    pl.semaphore_wait(barrier, len(greet))

    start_own(0)
    loads[1].wait()

    def columns(owner):
        return pl.ds(pl.multiple_of(owner * width, 128), width)

    def token_copy(owner, to, slot):
        return pltpu.make_async_remote_copy(
            src_ref=tok.at[:, columns(owner)],
            dst_ref=tok.at[:, columns(owner)],
            send_sem=tok_send.at[slot], recv_sem=tok_recv.at[owner],
            device_id={"tp": to}, device_id_type=MESH)

    across = [lax.rem(group + g, groups) * 2 + core for g in range(1, groups)]
    back = [lax.rem(group + groups - g, groups) * 2 + core for g in range(1, groups)]
    token_sends = [token_copy(me, to, i) for i, to in enumerate(across)]
    token_sends.append(token_copy(me, partner, groups - 1))
    for c in token_sends:
        c.start()
    loads[2].wait()
    down[own_rows, :] = stage[1].astype(jnp.bfloat16)

    arrived(0, z * 2 + 1 - y, extra)
    relay_own_extra(0, lambda c: c.start())
    step_sends(0, 1, lambda c: c.start(), True)

    relays = []
    for i, owner in enumerate(back):
        token_copy(owner, partner, groups + i).wait_recv()
        c = token_copy(owner, partner, groups + i)
        c.start()
        relays.append(c)
    token_copy(partner, partner, 0).wait_recv()
    for g in range(1, groups):
        token_copy(lax.rem(group + g, groups) * 2 + 1 - core, partner, 0).wait_recv()
    for c in token_sends + relays:
        c.wait_send()
    tile = 128

    @pl.loop(0, tokens // tile)
    def _(i):
        at = pl.ds(pl.multiple_of(i * tile, tile), tile)
        wide = tok[at, :].astype(jnp.float32)
        scale = lax.rsqrt(jnp.mean(wide * wide, axis=-1, keepdims=True) + epsilon)
        tok[at, :] = (wide * scale).astype(jnp.bfloat16)

    for d in range(2, chain):
        step_sends(0, d, lambda c: c.start(), True)
    start_own(1)
    for d in range(chain):
        side_arrivals(0, d)
    bm, bn = min(512, tokens), min(512, units)

    def expand(first, last):
        @pl.loop(first, last)
        def _(j):
            cols = pl.ds(pl.multiple_of(j * bn, bn), bn)

            @pl.loop(0, tokens // bm)
            def _(i):
                at = pl.ds(pl.multiple_of(i * bm, bm), bm)
                values = jnp.dot(tok[at, :], up[:, cols], preferred_element_type=jnp.float32)
                values = jnp.maximum(values, 0.0)
                hidden[at, cols] = (values * values).astype(jnp.bfloat16)

    expand(0, units // bn // 2)
    arrived(1, z * 2 + 1 - y, extra)
    relay_own_extra(1, lambda c: c.start())
    step_sends(1, 1, lambda c: c.start(), True)
    expand(units // bn // 2, units // bn)

    def pair_copy(r, h):
        return pltpu.make_async_remote_copy(
            src_ref=part.at[r, h], dst_ref=pair.at[r, h], send_sem=pair_send.at[r, h], recv_sem=pair_recv.at[r, h],
            device_id={"tp": partner}, device_id_type=MESH)

    def cross_copy(r, h, to_group, from_group):
        slot = r % per_owner
        return pltpu.make_async_remote_copy(
            src_ref=part.at[r, h], dst_ref=cross.at[from_group, slot, h],
            send_sem=cross_send.at[r, h], recv_sem=cross_recv.at[from_group, slot, h],
            device_id={"tp": to_group * 2 + core}, device_id_type=MESH)

    def multiply(r, hs):
        where = pl.ds(pl.multiple_of(r * rows + hs[0] * half_rows, 16), len(hs) * half_rows)

        @pl.loop(0, tokens // bm)
        def _(i):
            at = pl.ds(pl.multiple_of(i * bm, bm), bm)
            values = lax.dot_general(
                hidden[at, :], down[where, :], (((1,), (1,)), ((), ())),
                preferred_element_type=jnp.float32).astype(jnp.bfloat16)
            for i_h, h in enumerate(hs):
                part[r, h, at, :] = values[:, i_h * half_rows:(i_h + 1) * half_rows]

        @pl.when(r // per_owner % 2 != core)
        def _():
            for h in hs:
                pair_copy(r, h).start()

    def pair_sum(r, hs):
        owner = r // per_owner

        @pl.when(owner % 2 == core)
        def _():
            for h in hs:
                pair_copy(r, h).wait_recv()

                @pl.loop(0, tokens // tile)
                def _(i):
                    at = pl.ds(pl.multiple_of(i * tile, tile), tile)
                    both = part[r, h, at, :].astype(jnp.float32) + pair[r, h, at, :].astype(jnp.float32)
                    part[r, h, at, :] = both.astype(jnp.bfloat16)

                @pl.when(owner // 2 != group)
                def _():
                    cross_copy(r, h, owner // 2, group).start()

    def at_distance(d, flip, fn):
        for sign in (-1, 1):
            at = z + sign * d

            @pl.when((at >= 0) & (at < chain))
            def _():
                fn(at * 2 + (y + flip) % 2)

    every = list(range(halves))

    def side_block(r):
        for h in every:
            arrived(1, r, h)
            multiply(r, [h])
            pair_sum(r, [h])

    multiply(fs, every)
    side_block(z * 2 + 1 - y)
    pair_sum(fs, every)
    at_distance(1, 0, lambda r: multiply(r, every))

    @pl.loop(2, chain)
    def _(d):
        step_sends(1, d, lambda c: c.start(), True)
        at_distance(d - 1, 0, lambda r: pair_sum(r, every))
        at_distance(d - 1, 1, side_block)
        at_distance(d, 0, lambda r: multiply(r, every))

    at_distance(chain - 1, 0, lambda r: pair_sum(r, every))
    at_distance(chain - 1, 1, side_block)

    for s in range(per_owner):
        r = me * per_owner + s
        for h in every:
            for g in range(1, groups):
                other = lax.rem(group + g, groups)
                cross_copy(r, h, other, other).wait_recv()

            @pl.loop(0, tokens // tile)
            def _(i):
                at = pl.ds(pl.multiple_of(i * tile, tile), tile)
                value = part[r, h, at, :].astype(jnp.float32)
                for g in range(1, groups):
                    value = value + cross[lax.rem(group + g, groups), s, h, at, :].astype(jnp.float32)
                first = s * rows + h * half_rows
                total[at, first:first + half_rows] = value.astype(jnp.bfloat16)

    for m in (0, 1):
        for way, k in own_sends(m):
            when_way(way, lambda way=way, k=k: copy(m, fs, k, way).wait_send())
        relay_own_extra(m, lambda c: c.wait_send())

        @pl.loop(1, chain)
        def _(d):
            step_sends(m, d, lambda c: c.wait_send(), False)

    @pl.loop(0, n)
    def _(r):
        owner = r // per_owner

        @pl.when(owner % 2 != core)
        def _():
            for h in every:
                pair_copy(r, h).wait_send()

        @pl.when((owner % 2 == core) & (owner // 2 != group))
        def _():
            for h in every:
                cross_copy(r, h, owner // 2, group).wait_send()


def on_device(n, tp, tokens, norm_gain, up_weight, down_weight):
    rows, units = up_weight.shape
    count, width = tokens.shape
    bf16 = jnp.bfloat16
    groups, per_owner = tp // 2, n // tp
    chunks = len(chunks_of(rows, 0))
    halves = chunks - 1
    half_rows = rows // halves
    features = width * tp
    dma = pltpu.SemaphoreType.DMA
    flops = 2 * 2 * count * features * units
    return tuple(pl.pallas_call(
        functools.partial(kernel, n, tp),
        out_shape=(pltpu.VMEM((features, units), bf16), pltpu.VMEM((features, units), bf16),
                   pltpu.VMEM((count, width), bf16)),
        in_specs=[pl.BlockSpec(memory_space=pl.ANY if i != 1 else pltpu.VMEM) for i in range(4)],
        out_specs=[pl.BlockSpec(memory_space=pltpu.VMEM)] * 3,
        scratch_shapes=[
            pltpu.VMEM((2, rows, units), jnp.float32),
            pltpu.VMEM((count, features), bf16),
            pltpu.VMEM((count, units), bf16),
            pltpu.VMEM((n, halves, count, half_rows), bf16),
            pltpu.VMEM((n, halves, count, half_rows), bf16),
            pltpu.VMEM((groups, per_owner, halves, count, half_rows), bf16),
            dma((2, 3, n, chunks)), dma((2, n, chunks)),
            dma((2 * groups,)), dma((tp,)),
            dma((n, halves)), dma((n, halves)), dma((n, halves)), dma((groups, per_owner, halves)),
            dma((3,)),
        ],
        cost_estimate=pl.CostEstimate(flops=flops, bytes_accessed=4 * features * units * 2, transcendentals=0),
        compiler_params=pltpu.CompilerParams(
            collective_id=0, has_side_effects=True, vmem_limit_bytes=44 << 20),
    )(tokens, norm_gain[None, :], up_weight, down_weight))


def solution(mesh):
    return jax.shard_map(
        functools.partial(on_device, mesh.shape["fs"], mesh.shape["tp"]),
        mesh=mesh,
        in_specs=(P("fs", "tp"), P("fs"), P("fs", "tp"), P("fs", "tp")),
        out_specs=(P(None, "tp"), P(None, "tp"), P("fs", "tp")),
        check_vma=False,
    )
```
